32 devices in a mesh: fs: 8 (over z, y), tp: 4 (over x, core).
Axes of the slice: x: 2, y: 2, z: 4, core: 2. Of those that a mesh axis runs over, the one named last changes fastest.
Arguments:
- tokens: bfloat16 [4096, 2048], P('fs', 'tp'), may hold values from -6 to 6
- mixer_gain: float32 [2048], replicated, may hold values from 0.1 to 1.9
- recur_in: bfloat16 [2048, 1024], P('fs', 'tp'), may hold values from -0.125 to 0.125
- branch_in: bfloat16 [2048, 1024], P('fs', 'tp'), may hold values from -0.125 to 0.125
- conv_taps: bfloat16 [4, 1024], replicated, may hold values from -3 to 3
- recur_gate: bfloat16 [2, 16, 64, 64], replicated, may hold values from -0.75 to 0.75
- input_gate: bfloat16 [2, 16, 64, 64], replicated, may hold values from -0.75 to 0.75
- decay_param: float32 [2, 1024], replicated, may hold values from 3.5 to 11
- recur_gain: float32 [1024], replicated, may hold values from 0.1 to 1.9
- recur_out: bfloat16 [1024, 2048], P('tp', 'fs'), may hold values from -0.1875 to 0.1875
- mixer_post: float32 [2048], replicated, may hold values from 0.1 to 1.9
- channel_gain: float32 [2048], replicated, may hold values from 0.1 to 1.9
- hidden_gate: bfloat16 [2048, 5632], P('fs', 'tp'), may hold values from -0.125 to 0.125
- hidden_up: bfloat16 [2048, 5632], P('fs', 'tp'), may hold values from -0.125 to 0.125
- hidden_down: bfloat16 [5632, 2048], P('tp', 'fs'), may hold values from -0.078125 to 0.078125
- channel_post: float32 [2048], replicated, may hold values from 0.1 to 1.9
Outputs:
- layer_out: bfloat16 [4096, 2048], P('fs', 'tp')
The draws below stay inside these ranges and needn't reach their ends.
All inputs are finite; a program needn't handle non-finite values.
Results may differ from the reference program's by a relative error of at most 0.018.
Values may be sent and summed in bfloat16 or wider, within the bound.
A program may use at most 64 MiB of HBM per device.

```python
import math
import jax
import jax.numpy as jnp
from jax import lax

D = 2048
RNN = 1024
BLOCK = 64
CONV = 4
FF = 5632
TOK_DEV = 512
BLOCKS = 16
TOKENS = 4096
PARTS_SIZE = 4
N_FS = 8


def draw_tokens(key, part):
    base_key = jax.random.fold_in(key, 11)
    span_key = jax.random.fold_in(key, 12)
    span_count = (TOKENS + 31) // 32
    base_draw = jnp.clip(jax.random.normal(base_key, (TOKENS, D), jnp.float32), -4.0, 4.0)
    offset = jnp.clip(jax.random.normal(span_key, (span_count, D), jnp.float32), -2.0, 2.0)
    shifted = base_draw + jnp.repeat(offset, 32, axis=0)[:TOKENS]
    return shifted.astype(jnp.bfloat16)


def draw_decay_param(key, part):
    pick_key = jax.random.fold_in(key, 21)
    slow_key = jax.random.fold_in(key, 22)
    fast_key = jax.random.fold_in(key, 23)
    slow_share = 0.5
    slow_mask = jax.random.uniform(pick_key, (2, RNN), jnp.float32) < slow_share
    slow_rate = jnp.exp(jax.random.uniform(slow_key, (2, RNN), jnp.float32, math.log(0.05 / TOK_DEV), math.log(0.3 / TOK_DEV)))
    fast_rate = jnp.exp(jax.random.uniform(fast_key, (2, RNN), jnp.float32, math.log(1.0 / 400.0), math.log(1.0 / 120.0)))
    chosen = jnp.where(slow_mask, slow_rate, fast_rate)
    return (-jnp.log(jnp.expm1(chosen))).astype(jnp.float32)


def level_of(stream_key, dims, pieces, smallest, high):
    def one(axis_at, blocks):
        steps = jax.random.uniform(jax.random.fold_in(jax.random.fold_in(stream_key, 6), axis_at), (blocks,), jnp.float32, smallest / len(pieces), high / len(pieces))
        return jnp.repeat(jnp.exp(steps), dims[axis_at] // blocks).reshape((-1,) + (1,) * (len(dims) - axis_at - 1))

    level = one(*pieces[0])
    for cut in pieces[1:]:
        level = level * one(*cut)
    return level


def noise(key, extent, deviation, most, cuts=(), dtype=jnp.bfloat16):
    drawn = deviation * jax.random.normal(key, extent, jnp.float32)
    if cuts:
        drawn = drawn * level_of(key, extent, cuts, -0.22, 0.18)
    return jnp.clip(drawn, -most, most).astype(dtype)


def setup_inputs(seed: int = 0) -> dict:
    arg_keys = jax.random.split(jax.random.key(seed), 17)
    tokens = draw_tokens(jax.random.fold_in(arg_keys[16], 71), 0)
    mixer_gain = jnp.clip(1.0 + 0.18 * jax.random.normal(arg_keys[1], (D,), jnp.float32), 0.1, 1.9)
    recur_in = noise(arg_keys[2], (D, RNN), D ** -0.5, 0.125, ((0, 8), (1, 4)))
    branch_in = noise(arg_keys[3], (D, RNN), D ** -0.5, 0.125, ((0, 8), (1, 4)))
    conv_taps = noise(arg_keys[4], (CONV, RNN), CONV ** -0.5, 3.0)
    recur_gate = noise(arg_keys[5], (2, BLOCKS, BLOCK, BLOCK), BLOCK ** -0.5, 0.75)
    input_gate = noise(arg_keys[6], (2, BLOCKS, BLOCK, BLOCK), BLOCK ** -0.5, 0.75)
    decay_param = draw_decay_param(jax.random.fold_in(arg_keys[16], 71), 0)
    recur_gain = jnp.clip(1.0 + 0.18 * jax.random.normal(arg_keys[8], (RNN,), jnp.float32), 0.1, 1.9)
    recur_out = noise(arg_keys[9], (RNN, D), RNN ** -0.5, 0.1875, ((0, 4), (1, 8)))
    mixer_post = jnp.clip(1.0 + 0.18 * jax.random.normal(arg_keys[10], (D,), jnp.float32), 0.1, 1.9)
    channel_gain = jnp.clip(1.0 + 0.18 * jax.random.normal(arg_keys[11], (D,), jnp.float32), 0.1, 1.9)
    hidden_gate = noise(arg_keys[12], (D, FF), D ** -0.5, 0.125, ((0, 8), (1, 4)))
    hidden_up = noise(arg_keys[13], (D, FF), D ** -0.5, 0.125, ((0, 8), (1, 4)))
    hidden_down = noise(arg_keys[14], (FF, D), FF ** -0.5, 0.078125, ((0, 4), (1, 8)))
    channel_post = jnp.clip(1.0 + 0.18 * jax.random.normal(arg_keys[15], (D,), jnp.float32), 0.1, 1.9)
    return {"tokens": tokens, "mixer_gain": mixer_gain, "recur_in": recur_in, "branch_in": branch_in, "conv_taps": conv_taps, "recur_gate": recur_gate, "input_gate": input_gate, "decay_param": decay_param, "recur_gain": recur_gain, "recur_out": recur_out, "mixer_post": mixer_post, "channel_gain": channel_gain, "hidden_gate": hidden_gate, "hidden_up": hidden_up, "hidden_down": hidden_down, "channel_post": channel_post}


EPS = 1e-06
SHRINK = 8.0

def rms_scale(values, gain):
    return values * lax.rsqrt(lax.optimization_barrier(jnp.mean(values * values, axis=-1, keepdims=True)) + EPS) * gain

def linear_scan(decay, inflow, reverse):

    def combine(former, latter):
        return (former[0] * latter[0], latter[0] * former[1] + latter[1])
    return lax.associative_scan(combine, (decay, inflow), axis=0, reverse=reverse)[1]

def short_conv(recur_x, taps):
    length = recur_x.shape[0]
    padded = jnp.pad(recur_x.astype(jnp.float32), ((2, 1), (0, 0)))
    total = taps[0] * padded[0:length]
    for position in range(1, taps.shape[0]):
        total = total + taps[position] * padded[position:position + length]
    return total

def recurrence(conv_out, rate_weight, inlet_weight, decay_row, reverse):
    length, width = conv_out.shape
    grouped = conv_out.reshape(length, rate_weight.shape[0], rate_weight.shape[1])
    rate = jax.nn.sigmoid(jnp.einsum('lhi,hij->lhj', grouped, rate_weight.astype(jnp.float32), precision=lax.Precision.HIGHEST).reshape(length, width))
    inlet = jax.nn.sigmoid(jnp.einsum('lhi,hij->lhj', grouped, inlet_weight.astype(jnp.float32), precision=lax.Precision.HIGHEST).reshape(length, width))
    log_decay = -SHRINK * rate * jax.nn.softplus(-decay_row)
    inflow = conv_out * inlet * jnp.sqrt(-jnp.expm1(2.0 * log_decay))
    return linear_scan(jnp.exp(log_decay), inflow, reverse)

def grouped_product(left, right, groups):
    length = left.shape[0]
    inner = left.shape[1] // groups
    left_groups = left.astype(jnp.float32).reshape(length, groups, inner)
    right_groups = right.astype(jnp.float32).reshape(groups, inner, right.shape[1])
    partial_value = jnp.einsum('lgk,gkd->gld', left_groups, right_groups, precision=lax.Precision.HIGHEST)
    rounded = lax.optimization_barrier(partial_value.astype(jnp.bfloat16))
    return lax.optimization_barrier(jnp.sum(rounded.astype(jnp.float32), axis=0))

def reference(tokens, mixer_gain, recur_in, branch_in, conv_taps, recur_gate, input_gate, decay_param, recur_gain, recur_out, mixer_post, channel_gain, hidden_gate, hidden_up, hidden_down, channel_post):
    taps = conv_taps.astype(jnp.float32)

    def one_sequence(sequence):
        seq_float = sequence.astype(jnp.float32)
        normed_in = rms_scale(seq_float, mixer_gain).astype(jnp.bfloat16)
        recur_x = jnp.dot(normed_in, recur_in, preferred_element_type=jnp.float32).astype(jnp.bfloat16)
        branch_x = jnp.dot(normed_in, branch_in, preferred_element_type=jnp.float32).astype(jnp.bfloat16)
        conv_out = short_conv(recur_x, taps)
        forward = recurrence(conv_out, recur_gate[0], input_gate[0], decay_param[0], False)
        backward = recurrence(conv_out, recur_gate[1], input_gate[1], decay_param[1], True)
        mixed = (forward + backward) * jax.nn.gelu(branch_x.astype(jnp.float32))
        recur_y = (mixed * recur_gain).astype(jnp.bfloat16)
        branch_sum = grouped_product(recur_y, recur_out, PARTS_SIZE)
        res_mid = (seq_float + rms_scale(branch_sum, mixer_post)).astype(jnp.bfloat16)
        mid_float = res_mid.astype(jnp.float32)
        channel_in = rms_scale(mid_float, channel_gain).astype(jnp.bfloat16)
        gate = jnp.dot(channel_in, hidden_gate, preferred_element_type=jnp.float32)
        up_value = jnp.dot(channel_in, hidden_up, preferred_element_type=jnp.float32)
        hidden = (jax.nn.silu(gate) * up_value).astype(jnp.bfloat16)
        hidden_sum = grouped_product(hidden, hidden_down, PARTS_SIZE)
        return (mid_float + rms_scale(hidden_sum, channel_post)).astype(jnp.bfloat16)
    result = lax.map(one_sequence, tokens.reshape(N_FS, TOK_DEV, D))
    return result.reshape(N_FS * TOK_DEV, D)
```

```python
import functools

import jax
import jax.numpy as jnp
from jax import lax
from jax.experimental import pallas as pl
from jax.experimental.pallas import tpu as pltpu
from jax.sharding import PartitionSpec as P

EPS = 1e-06
SHRINK = 8.0
CORES = 2


def rms_scale(values, gain):
    return values * lax.rsqrt(jnp.mean(values * values, axis=-1, keepdims=True) + EPS) * gain


def snake_order(mesh):
    count = mesh.shape["fs"]
    axis = list(mesh.axis_names).index("fs")
    line = mesh.devices.take(0, axis=1 - axis).reshape(-1)
    where = [getattr(device, "coords", None) for device in line]
    if any(spot is None for spot in where):
        return list(range(count))
    at = {}
    for index, spot in enumerate(where):
        at[(spot[2], spot[1])] = index
    depth = 1 + max(z for z, _ in at)
    width = 1 + max(y for _, y in at)
    if depth * width != count or len(at) != count or width < 2 or depth % 2:
        return list(range(count))
    order = [at[(z, 0)] for z in range(depth)]
    for back, z in enumerate(reversed(range(depth))):
        columns = range(1, width)
        order += [at[(z, y)] for y in (columns if back % 2 == 0 else reversed(columns))]
    return order


class Ring:
    def __init__(self, order):
        self.n = len(order)
        self.order = order
        n = self.n
        self.pairs = {
            1: [(order[p], order[(p + 1) % n]) for p in range(n)],
            -1: [(order[p], order[(p - 1) % n]) for p in range(n)],
        }
        place = [0] * n
        for p, index in enumerate(order):
            place[index] = p
        self.order_row = jnp.array(order, jnp.int32)
        self.here = jnp.array(place, jnp.int32)[lax.axis_index("fs")]
        self.landed = {1: [], -1: []}

    def source(self, step):
        return self.order_row[lax.rem(self.here - step + self.n, self.n)]

    def send(self, value, way):
        landed = self.landed[way]
        if len(landed) >= 2:
            value = lax.optimization_barrier((value, landed[-2]))[0]
        value = lax.ppermute(value, "fs", self.pairs[way])
        landed.append(value)
        return value

    def gather(self, shards):
        n = self.n
        found = [[(self.source(0), shard)] for shard in shards]
        heads = [{1: shard, -1: shard} for shard in shards]
        for step in range(1, n // 2 + 1):
            for index in range(len(shards)):
                for way in (1, -1):
                    steps = n // 2 if (way == 1) == (index % 2 == 0) else n - 1 - n // 2
                    if step <= steps:
                        heads[index][way] = self.send(heads[index][way], way)
                        found[index].append((self.source(way * step), heads[index][way]))
        return found


def stack_rows(blocks):
    height, width = blocks[0][1].shape
    total = jnp.zeros((height * len(blocks), width), blocks[0][1].dtype)
    for source, block in blocks:
        total = lax.dynamic_update_slice(total, block, (source * height, 0))
    return total


def stack_columns(blocks):
    height, width = blocks[0][1].shape
    total = jnp.zeros((height, width * len(blocks)), blocks[0][1].dtype)
    for source, block in blocks:
        total = lax.dynamic_update_slice(total, block, (0, source * width))
    return total


def swap_cores(value, count):
    return lax.ppermute(value, "tp", [(t, t ^ 1) for t in range(count)])


def from_chip(value, shift, count):
    return lax.ppermute(value, "tp", [(t, (t + CORES * shift) % count) for t in range(count)])


def chips_shares(value, count):
    chips = count // CORES
    chip = lax.axis_index("tp") // CORES
    found = [(chip, value)]
    for shift in range(1, chips):
        found.append((lax.rem(chip - shift + chips, chips), from_chip(value, shift, count)))
    return found


def gather_features(value, count):
    core = lax.rem(lax.axis_index("tp"), CORES)
    width = value.shape[1]
    total = jnp.zeros((value.shape[0], width * count), value.dtype)
    for chip, block in chips_shares(value, count):
        other = swap_cores(block, count)
        total = lax.dynamic_update_slice(total, block, (0, (chip * CORES + core) * width))
        total = lax.dynamic_update_slice(total, other, (0, (chip * CORES + 1 - core) * width))
    return total


def sum_all(value, count):
    core = lax.rem(lax.axis_index("tp"), CORES)
    half = value.shape[1] // CORES
    keep = lax.dynamic_slice_in_dim(value, core * half, half, 1)
    give = lax.dynamic_slice_in_dim(value, (1 - core) * half, half, 1)
    chip_sum = keep.astype(jnp.float32) + swap_cores(give, count).astype(jnp.float32)
    chip_sum = chip_sum.astype(jnp.bfloat16)
    total = 0.0
    for _, block in chips_shares(chip_sum, count):
        total = total + block.astype(jnp.float32)
    mine = total.astype(jnp.bfloat16)
    other = swap_cores(mine, count)
    low = jnp.where(core == 0, mine, other)
    high = jnp.where(core == 0, other, mine)
    return jnp.concatenate([low, high], axis=1)


def sum_own(value, count):
    rank = lax.axis_index("tp")
    core = lax.rem(rank, CORES)
    chip = rank // CORES
    chips = count // CORES
    length = value.shape[0]
    width = value.shape[1] // count

    def block(chip_at, core_at):
        at = (chip_at * CORES + core_at) * width
        return lax.dynamic_slice_in_dim(value, at, width, 1)

    total = 0.0
    for shift in list(range(1, chips)) + [0]:
        target = lax.rem(chip + shift, chips)
        part = block(target, core).astype(jnp.float32)
        part = part + swap_cores(block(target, 1 - core), count).astype(jnp.float32)
        if shift:
            part = from_chip(part.astype(jnp.bfloat16), shift, count).astype(jnp.float32)
        total = total + part
    return total


def minus_expm1(value):
    series = jnp.ones_like(value)
    for order in range(9, 1, -1):
        series = 1.0 + value * (1.0 / order) * series
    return jnp.where(value > -0.5, -value * series, 1.0 - jnp.exp(value))


def scan_block(decay, inflow, reverse):
    length = decay.shape[0]
    row = lax.broadcasted_iota(jnp.int32, decay.shape, 0)
    reach = 1
    while reach < length:
        if reverse:
            inside = row < length - reach
            turn = length - reach
        else:
            inside = row >= reach
            turn = reach
        before_inflow = jnp.where(inside, pltpu.roll(inflow, turn, 0), 0.0)
        inflow = inflow + decay * before_inflow
        if 2 * reach < length:
            decay = decay * jnp.where(inside, pltpu.roll(decay, turn, 0), 1.0)
        reach *= 2
    return inflow


def mixer_kernel(recur_ref, branch_ref, taps_ref, gate_ref, decay_ref, gain_ref, out_ref):
    recur = recur_ref[...].astype(jnp.float32)
    length, width = recur.shape
    row = lax.broadcasted_iota(jnp.int32, recur.shape, 0)
    taps = taps_ref[...]
    conv = taps[2:3] * recur
    for tap, shift in ((0, 2), (1, 1), (3, length - 1)):
        inside = row < length - 1 if tap == 3 else row >= shift
        conv = conv + taps[tap : tap + 1] * jnp.where(inside, pltpu.roll(recur, shift, 0), 0.0)
    first = conv.astype(jnp.bfloat16)
    rest = conv - first.astype(jnp.float32)
    second = rest.astype(jnp.bfloat16)
    third = (rest - second.astype(jnp.float32)).astype(jnp.bfloat16)
    total = None
    for direction in range(2):
        logits = []
        for kind in range(2):
            weight = gate_ref[0, :, pl.ds((direction * 2 + kind) * width, width)]
            logits.append(
                jnp.dot(third, weight, preferred_element_type=jnp.float32)
                + jnp.dot(second, weight, preferred_element_type=jnp.float32)
                + jnp.dot(first, weight, preferred_element_type=jnp.float32)
            )
        rate = 1.0 / (1.0 + jnp.exp(-logits[0]))
        inlet = 1.0 / (1.0 + jnp.exp(-logits[1]))
        log_decay = rate * decay_ref[direction : direction + 1, :]
        inflow = conv * inlet * jnp.sqrt(minus_expm1(2.0 * log_decay))
        state = scan_block(jnp.exp(log_decay), inflow, direction == 1)
        total = state if total is None else total + state
    branch = branch_ref[...].astype(jnp.float32)
    inner = 0.7978845608028654 * (branch + 0.044715 * (branch * branch * branch))
    gelu = branch * (0.5 * (1.0 + jnp.tanh(inner)))
    out_ref[...] = (total * gelu * gain_ref[...]).astype(jnp.bfloat16)


def mixer(recur_x, branch_x, taps, rate_own, inlet_own, decay_own, gain_own):
    length, channels = recur_x.shape
    group = rate_own.shape[-1]
    lanes = min(channels, 2 * group)
    blocks = channels // lanes
    per = lanes // group

    def dense(weight):
        spread = weight.reshape(2, blocks, per, group, 1, group) * jnp.eye(per, dtype=weight.dtype)[:, None, :, None]
        return spread.reshape(2, blocks, lanes, lanes)

    both = jnp.stack([dense(rate_own), dense(inlet_own)], axis=1)
    gates = both.transpose(2, 3, 0, 1, 4).reshape(blocks, lanes, 4 * lanes)
    slope = -SHRINK * jax.nn.softplus(-decay_own)
    column = lambda j: (0, j)
    return pl.pallas_call(
        mixer_kernel,
        grid=(blocks,),
        out_shape=jax.ShapeDtypeStruct((length, channels), jnp.bfloat16),
        in_specs=[
            pl.BlockSpec((length, lanes), column),
            pl.BlockSpec((length, lanes), column),
            pl.BlockSpec((taps.shape[0], lanes), column),
            pl.BlockSpec((1, lanes, 4 * lanes), lambda j: (j, 0, 0)),
            pl.BlockSpec((2, lanes), column),
            pl.BlockSpec((1, lanes), column),
        ],
        out_specs=pl.BlockSpec((length, lanes), column),
        cost_estimate=pl.CostEstimate(flops=int(3e9), bytes_accessed=2**20, transcendentals=2**21),
        compiler_params=pltpu.CompilerParams(vmem_limit_bytes=24 * 2**20),
    )(recur_x, branch_x, taps, gates, slope, gain_own.reshape(1, channels))


def on_device(
    order,
    tp_count,
    tokens,
    mixer_gain,
    recur_in,
    branch_in,
    conv_taps,
    recur_gate,
    input_gate,
    decay_param,
    recur_gain,
    recur_out,
    mixer_post,
    channel_gain,
    hidden_gate,
    hidden_up,
    hidden_down,
    channel_post,
):
    rank_tp = lax.axis_index("tp")
    feature_width = tokens.shape[1]
    model_width = mixer_gain.shape[0]
    channel_width = recur_in.shape[1]
    group_count = channel_width // recur_gate.shape[-1]
    feature_start = rank_tp * feature_width
    channel_start = rank_tp * channel_width

    ring = Ring(order)
    recur_blocks, branch_blocks = ring.gather([recur_in, branch_in])
    (out_blocks,) = ring.gather([recur_out])
    gate_blocks, up_blocks = ring.gather([hidden_gate, hidden_up])
    half = hidden_down.shape[0] // 2
    down_low, down_high = ring.gather([hidden_down[:half], hidden_down[half:]])

    gathered_in = gather_features(tokens, tp_count)
    gathered_float = gathered_in.astype(jnp.float32)
    normed_in = rms_scale(gathered_float, mixer_gain).astype(jnp.bfloat16)
    recur_x = jnp.dot(normed_in, stack_rows(recur_blocks), preferred_element_type=jnp.float32).astype(jnp.bfloat16)
    branch_x = jnp.dot(normed_in, stack_rows(branch_blocks), preferred_element_type=jnp.float32).astype(jnp.bfloat16)

    taps = lax.dynamic_slice_in_dim(conv_taps, channel_start, channel_width, 1).astype(jnp.float32)
    group_start = rank_tp * group_count
    rate_own = lax.dynamic_slice_in_dim(recur_gate, group_start, group_count, 1)
    inlet_own = lax.dynamic_slice_in_dim(input_gate, group_start, group_count, 1)
    decay_own = lax.dynamic_slice_in_dim(decay_param, channel_start, channel_width, 1)
    gain_own = lax.dynamic_slice_in_dim(recur_gain, channel_start, channel_width, 0)
    recur_y = mixer(recur_x, branch_x, taps, rate_own, inlet_own, decay_own, gain_own)

    branch_part = jnp.dot(recur_y, stack_columns(out_blocks), preferred_element_type=jnp.float32)
    branch_sum = sum_all(branch_part.astype(jnp.bfloat16), tp_count).astype(jnp.float32)
    mid_full = (gathered_float + rms_scale(branch_sum, mixer_post)).astype(jnp.bfloat16)
    mid_own = lax.dynamic_slice_in_dim(mid_full, feature_start, feature_width, 1)
    channel_in = rms_scale(mid_full.astype(jnp.float32), channel_gain).astype(jnp.bfloat16)

    gate_total = jnp.dot(channel_in, stack_rows(gate_blocks), preferred_element_type=jnp.float32)
    up_total = jnp.dot(channel_in, stack_rows(up_blocks), preferred_element_type=jnp.float32)
    hidden = (jax.nn.silu(gate_total) * up_total).astype(jnp.bfloat16)

    down = jnp.concatenate([stack_columns(down_low), stack_columns(down_high)], axis=0)
    hidden_part = jnp.dot(hidden, down, preferred_element_type=jnp.float32).astype(jnp.bfloat16)
    hidden_own = sum_own(hidden_part, tp_count)
    energy_own = jnp.sum(hidden_own * hidden_own, axis=1).reshape(-1, 128)
    hidden_energy = lax.psum(energy_own, "tp").reshape(-1)
    close_own = lax.dynamic_slice_in_dim(channel_post, feature_start, feature_width, 0)
    return (
        mid_own.astype(jnp.float32)
        + hidden_own * lax.rsqrt(hidden_energy / model_width + EPS)[:, None] * close_own
    ).astype(jnp.bfloat16)


def solution(mesh):
    in_specs = (
        P("fs", "tp"),
        P(),
        P("fs", "tp"),
        P("fs", "tp"),
        P(),
        P(),
        P(),
        P(),
        P(),
        P("tp", "fs"),
        P(),
        P(),
        P("fs", "tp"),
        P("fs", "tp"),
        P("tp", "fs"),
        P(),
    )
    out_specs = P("fs", "tp")
    body = functools.partial(on_device, snake_order(mesh), mesh.shape["tp"])
    return jax.shard_map(body, mesh=mesh, in_specs=in_specs, out_specs=out_specs, check_vma=False)
```

```python
import functools

import jax
import jax.numpy as jnp
from jax import lax
from jax.experimental import pallas as pl
from jax.experimental.pallas import tpu as pltpu
from jax.sharding import PartitionSpec as P

EPS = 1e-06
SHRINK = 8.0
CORES = 2
FLIGHT = 5


def rms_scale(values, gain):
    return values * lax.rsqrt(jnp.mean(values * values, axis=-1, keepdims=True) + EPS) * gain


def snake_order(mesh):
    count = mesh.shape["fs"]
    axis = list(mesh.axis_names).index("fs")
    line = mesh.devices.take(0, axis=1 - axis).reshape(-1)
    where = [getattr(device, "coords", None) for device in line]
    if any(spot is None for spot in where):
        return list(range(count))
    at = {}
    for index, spot in enumerate(where):
        at[(spot[2], spot[1])] = index
    depth = 1 + max(z for z, _ in at)
    width = 1 + max(y for _, y in at)
    if depth * width != count or len(at) != count or width < 2 or depth % 2:
        return list(range(count))
    order = [at[(z, 0)] for z in range(depth)]
    for back, z in enumerate(reversed(range(depth))):
        columns = range(1, width)
        order += [at[(z, y)] for y in (columns if back % 2 == 0 else reversed(columns))]
    return order


class Ring:
    def __init__(self, order):
        self.n = len(order)
        self.order = order
        n = self.n
        self.pairs = {
            1: [(order[p], order[(p + 1) % n]) for p in range(n)],
            -1: [(order[p], order[(p - 1) % n]) for p in range(n)],
        }
        place = [0] * n
        for p, index in enumerate(order):
            place[index] = p
        self.order_row = jnp.array(order, jnp.int32)
        self.here = jnp.array(place, jnp.int32)[lax.axis_index("fs")]
        self.landed = {1: [], -1: []}

    def source(self, step):
        return self.order_row[lax.rem(self.here - step + self.n, self.n)]

    def send(self, value, way):
        landed = self.landed[way]
        if len(landed) >= FLIGHT:
            value = lax.optimization_barrier((value, landed[-FLIGHT]))[0]
        value = lax.ppermute(value, "fs", self.pairs[way])
        landed.append(value)
        return value

    def gather(self, shards, ties={}, paired=False, lead=1):
        n = self.n
        found = [[(self.source(0), shard)] for shard in shards]
        heads = [{1: shard, -1: shard} for shard in shards]
        for step in range(1, n // 2 + 1):
            for index in range(len(shards)):
                for way in (1, -1):
                    steps = n // 2 if (way == lead) == (index % 2 == 0 or paired) else n - 1 - n // 2
                    if step <= steps:
                        if step in ties:
                            heads[index][way] = lax.optimization_barrier((heads[index][way], ties[step]))[0]
                        heads[index][way] = self.send(heads[index][way], way)
                        found[index].append((self.source(way * step), heads[index][way]))
        return found


def stack_rows(blocks):
    height, width = blocks[0][1].shape
    total = jnp.zeros((height * len(blocks), width), blocks[0][1].dtype)
    for source, block in blocks:
        total = lax.dynamic_update_slice(total, block, (source * height, 0))
    return total


def stack_columns(blocks):
    height, width = blocks[0][1].shape
    total = jnp.zeros((height, width * len(blocks)), blocks[0][1].dtype)
    for source, block in blocks:
        total = lax.dynamic_update_slice(total, block, (0, source * width))
    return total


def swap_cores(value, count):
    return lax.ppermute(value, "tp", [(t, t ^ 1) for t in range(count)])


def from_chip(value, shift, count):
    return lax.ppermute(value, "tp", [(t, (t + CORES * shift) % count) for t in range(count)])


def chips_shares(value, count):
    chips = count // CORES
    chip = lax.axis_index("tp") // CORES
    found = [(chip, value)]
    for shift in range(1, chips):
        found.append((lax.rem(chip - shift + chips, chips), from_chip(value, shift, count)))
    return found


def gather_features(value, count):
    core = lax.rem(lax.axis_index("tp"), CORES)
    width = value.shape[1]
    total = jnp.zeros((value.shape[0], width * count), value.dtype)
    for chip, block in chips_shares(value, count):
        other = swap_cores(block, count)
        total = lax.dynamic_update_slice(total, block, (0, (chip * CORES + core) * width))
        total = lax.dynamic_update_slice(total, other, (0, (chip * CORES + 1 - core) * width))
    return total


def sum_all(value, count):
    core = lax.rem(lax.axis_index("tp"), CORES)
    half = value.shape[1] // CORES
    keep = lax.dynamic_slice_in_dim(value, core * half, half, 1)
    give = lax.dynamic_slice_in_dim(value, (1 - core) * half, half, 1)
    chip_sum = keep.astype(jnp.float32) + swap_cores(give, count).astype(jnp.float32)
    chip_sum = chip_sum.astype(jnp.bfloat16)
    total = 0.0
    for _, block in chips_shares(chip_sum, count):
        total = total + block.astype(jnp.float32)
    mine = total.astype(jnp.bfloat16)
    other = swap_cores(mine, count)
    low = jnp.where(core == 0, mine, other)
    high = jnp.where(core == 0, other, mine)
    return jnp.concatenate([low, high], axis=1)


def sum_own(value, count):
    rank = lax.axis_index("tp")
    core = lax.rem(rank, CORES)
    chip = rank // CORES
    chips = count // CORES
    length = value.shape[0]
    width = value.shape[1] // count

    def block(chip_at, core_at):
        at = (chip_at * CORES + core_at) * width
        return lax.dynamic_slice_in_dim(value, at, width, 1)

    total = 0.0
    for shift in list(range(1, chips)) + [0]:
        target = lax.rem(chip + shift, chips)
        part = block(target, core).astype(jnp.float32)
        part = part + swap_cores(block(target, 1 - core), count).astype(jnp.float32)
        if shift:
            part = from_chip(part.astype(jnp.bfloat16), shift, count).astype(jnp.float32)
        total = total + part
    return total


def minus_expm1(value):
    series = jnp.ones_like(value)
    for order in range(9, 1, -1):
        series = 1.0 + value * (1.0 / order) * series
    return jnp.where(value > -0.5, -value * series, 1.0 - jnp.exp(value))


def scan_block(decay, inflow, reverse):
    length = decay.shape[0]
    row = lax.broadcasted_iota(jnp.int32, decay.shape, 0)
    reach = 1
    while reach < length:
        if reverse:
            inside = row < length - reach
            turn = length - reach
        else:
            inside = row >= reach
            turn = reach
        before_inflow = jnp.where(inside, pltpu.roll(inflow, turn, 0), 0.0)
        inflow = inflow + decay * before_inflow
        if 2 * reach < length:
            decay = decay * jnp.where(inside, pltpu.roll(decay, turn, 0), 1.0)
        reach *= 2
    return inflow


def mixer_kernel(recur_ref, branch_ref, taps_ref, gate_ref, decay_ref, gain_ref, out_ref):
    recur = recur_ref[...].astype(jnp.float32)
    length, width = recur.shape
    row = lax.broadcasted_iota(jnp.int32, recur.shape, 0)
    taps = taps_ref[...]
    conv = taps[2:3] * recur
    for tap, shift in ((0, 2), (1, 1), (3, length - 1)):
        inside = row < length - 1 if tap == 3 else row >= shift
        conv = conv + taps[tap : tap + 1] * jnp.where(inside, pltpu.roll(recur, shift, 0), 0.0)
    first = conv.astype(jnp.bfloat16)
    rest = conv - first.astype(jnp.float32)
    second = rest.astype(jnp.bfloat16)
    third = (rest - second.astype(jnp.float32)).astype(jnp.bfloat16)
    total = None
    for direction in range(2):
        logits = []
        for kind in range(2):
            weight = gate_ref[0, :, pl.ds((direction * 2 + kind) * width, width)]
            logits.append(
                jnp.dot(third, weight, preferred_element_type=jnp.float32)
                + jnp.dot(second, weight, preferred_element_type=jnp.float32)
                + jnp.dot(first, weight, preferred_element_type=jnp.float32)
            )
        rate = 1.0 / (1.0 + jnp.exp(-logits[0]))
        inlet = 1.0 / (1.0 + jnp.exp(-logits[1]))
        log_decay = rate * decay_ref[direction : direction + 1, :]
        inflow = conv * inlet * jnp.sqrt(minus_expm1(2.0 * log_decay))
        state = scan_block(jnp.exp(log_decay), inflow, direction == 1)
        total = state if total is None else total + state
    branch = branch_ref[...].astype(jnp.float32)
    inner = 0.7978845608028654 * (branch + 0.044715 * (branch * branch * branch))
    gelu = branch * (0.5 * (1.0 + jnp.tanh(inner)))
    out_ref[...] = (total * gelu * gain_ref[...]).astype(jnp.bfloat16)


def mixer(both_x, taps, rate_own, inlet_own, decay_own, gain_own):
    length, channels = both_x.shape[0], both_x.shape[1] // 2
    group = rate_own.shape[-1]
    lanes = min(channels, 2 * group)
    blocks = channels // lanes
    per = lanes // group

    def dense(weight):
        spread = weight.reshape(2, blocks, per, group, 1, group) * jnp.eye(per, dtype=weight.dtype)[:, None, :, None]
        return spread.reshape(2, blocks, lanes, lanes)

    both = jnp.stack([dense(rate_own), dense(inlet_own)], axis=1)
    gates = both.transpose(2, 3, 0, 1, 4).reshape(blocks, lanes, 4 * lanes)
    slope = -SHRINK * jax.nn.softplus(-decay_own)
    column = lambda j: (0, j)
    return pl.pallas_call(
        mixer_kernel,
        grid=(blocks,),
        out_shape=jax.ShapeDtypeStruct((length, channels), jnp.bfloat16),
        in_specs=[
            pl.BlockSpec((length, lanes), column),
            pl.BlockSpec((length, lanes), lambda j: (0, blocks + j)),
            pl.BlockSpec((taps.shape[0], lanes), column),
            pl.BlockSpec((1, lanes, 4 * lanes), lambda j: (j, 0, 0)),
            pl.BlockSpec((2, lanes), column),
            pl.BlockSpec((1, lanes), column),
        ],
        out_specs=pl.BlockSpec((length, lanes), column),
        cost_estimate=pl.CostEstimate(flops=int(3e9), bytes_accessed=2**20, transcendentals=2**21),
        compiler_params=pltpu.CompilerParams(vmem_limit_bytes=24 * 2**20),
    )(both_x, both_x, taps, gates, slope, gain_own.reshape(1, channels))


def on_device(
    order,
    tp_count,
    tokens,
    mixer_gain,
    recur_in,
    branch_in,
    conv_taps,
    recur_gate,
    input_gate,
    decay_param,
    recur_gain,
    recur_out,
    mixer_post,
    channel_gain,
    hidden_gate,
    hidden_up,
    hidden_down,
    channel_post,
):
    rank_tp = lax.axis_index("tp")
    feature_width = tokens.shape[1]
    model_width = mixer_gain.shape[0]
    channel_width = recur_in.shape[1]
    group_count = channel_width // recur_gate.shape[-1]
    feature_start = rank_tp * feature_width
    channel_start = rank_tp * channel_width

    ring = Ring(order)
    packed = jnp.concatenate([recur_in, branch_in, recur_out.reshape(recur_in.shape)], axis=1)
    mix_blocks, gate_blocks = ring.gather([packed, hidden_gate])
    in_blocks = [(source, block[:, : 2 * channel_width]) for source, block in mix_blocks]
    out_blocks = [
        (source, block[:, 2 * channel_width :].reshape(recur_out.shape)) for source, block in mix_blocks
    ]

    gathered_in = gather_features(tokens, tp_count)
    gathered_float = gathered_in.astype(jnp.float32)
    normed_in = rms_scale(gathered_float, mixer_gain).astype(jnp.bfloat16)
    both_x = jnp.dot(normed_in, stack_rows(in_blocks), preferred_element_type=jnp.float32).astype(jnp.bfloat16)

    taps = lax.dynamic_slice_in_dim(conv_taps, channel_start, channel_width, 1).astype(jnp.float32)
    group_start = rank_tp * group_count
    rate_own = lax.dynamic_slice_in_dim(recur_gate, group_start, group_count, 1)
    inlet_own = lax.dynamic_slice_in_dim(input_gate, group_start, group_count, 1)
    decay_own = lax.dynamic_slice_in_dim(decay_param, channel_start, channel_width, 1)
    gain_own = lax.dynamic_slice_in_dim(recur_gain, channel_start, channel_width, 0)
    recur_y = mixer(both_x, taps, rate_own, inlet_own, decay_own, gain_own)

    (up_blocks,) = ring.gather([hidden_up], lead=-1)
    branch_part = jnp.dot(recur_y, stack_columns(out_blocks), preferred_element_type=jnp.float32)
    branch_sum = sum_all(branch_part.astype(jnp.bfloat16), tp_count).astype(jnp.float32)
    mid_full = (gathered_float + rms_scale(branch_sum, mixer_post)).astype(jnp.bfloat16)
    mid_own = lax.dynamic_slice_in_dim(mid_full, feature_start, feature_width, 1)
    channel_in = rms_scale(mid_full.astype(jnp.float32), channel_gain).astype(jnp.bfloat16)

    gate_total = jnp.dot(channel_in, stack_rows(gate_blocks), preferred_element_type=jnp.float32)
    up_total = jnp.dot(channel_in, stack_rows(up_blocks), preferred_element_type=jnp.float32)
    hidden = (jax.nn.silu(gate_total) * up_total).astype(jnp.bfloat16)

    cut = max(hidden_down.shape[0] // 256, 1) * 128
    low_blocks, high_blocks = ring.gather(
        [hidden_down[:cut], hidden_down[cut:]], {4: hidden}, True
    )
    part_blocks = []
    for (source, low), (_, high) in zip(low_blocks, high_blocks):
        part = jnp.dot(hidden[:, :cut], low, preferred_element_type=jnp.float32)
        part = part + jnp.dot(hidden[:, cut:], high, preferred_element_type=jnp.float32)
        part_blocks.append((source, part.astype(jnp.bfloat16)))
    hidden_part = stack_columns(part_blocks)
    hidden_own = sum_own(hidden_part, tp_count)
    energy_own = jnp.sum(hidden_own * hidden_own, axis=1).reshape(-1, 128)
    hidden_energy = lax.psum(energy_own, "tp").reshape(-1)
    close_own = lax.dynamic_slice_in_dim(channel_post, feature_start, feature_width, 0)
    return (
        mid_own.astype(jnp.float32)
        + hidden_own * lax.rsqrt(hidden_energy / model_width + EPS)[:, None] * close_own
    ).astype(jnp.bfloat16)


def solution(mesh):
    in_specs = (
        P("fs", "tp"),
        P(),
        P("fs", "tp"),
        P("fs", "tp"),
        P(),
        P(),
        P(),
        P(),
        P(),
        P("tp", "fs"),
        P(),
        P(),
        P("fs", "tp"),
        P("fs", "tp"),
        P("tp", "fs"),
        P(),
    )
    out_specs = P("fs", "tp")
    body = functools.partial(on_device, snake_order(mesh), mesh.shape["tp"])
    return jax.shard_map(body, mesh=mesh, in_specs=in_specs, out_specs=out_specs, check_vma=False)
```
